32 devices in a mesh: sp: 4 (over y, x), tp: 8 (over z, core).
Axes of the slice: x: 2, y: 2, z: 4, core: 2. Of those that a mesh axis runs over, the one named last changes fastest.
Arguments:
- query_heads: bfloat16 [4096, 2048], P('sp', 'tp'), may hold values from -256 to 256
- key_heads: bfloat16 [4096, 1024], P('sp', 'tp'), may hold values from -7 to 7
- value_heads: bfloat16 [4096, 1024], P('sp', 'tp'), may hold values from -6 to 6
- sink_logit: float32 [32], P('tp'), may hold values from 3 to 7
- residual: bfloat16 [4096, 2048], P(('sp', 'tp')), may hold values from -6 to 6
- out_weight: bfloat16 [2048, 2048], replicated, may hold values from -0.5 to 0.5
- norm_gain: float32 [2048], replicated, may hold values from 0.1 to 1.9
- routes: int32 [4096, 2], P('sp'), may hold values from 0 to 3, all different within a row; in each aligned block of 128 rows (0 to 127, 128 to 255, ...) at most 80 rows name the same one
- route_weight: float32 [4096, 2], P(('sp', 'tp')), may hold values from 0.2 to 1
- gate_weight: bfloat16 [4, 2048, 2048], P('sp', None, 'tp'), may hold values from -0.3125 to 0.3125
- up_weight: bfloat16 [4, 2048, 2048], P('sp', None, 'tp'), may hold values from -0.3125 to 0.3125
- down_weight: bfloat16 [4, 2048, 2048], P('sp', 'tp'), may hold values from -0.0625 to 0.0625
Outputs:
- updated: bfloat16 [4096, 2048], P(('sp', 'tp'))
The draws below stay inside these ranges and needn't reach their ends.
Inputs may be any that keep to these rules, and one draw needn't show every extreme that they name: `routes`: each row names 2 different experts. In each aligned block of 128 rows no expert is named more than 80 times, and in every draw some block names some expert exactly 80 times.
All inputs are finite; a program needn't handle non-finite values.
Results may differ from the reference program's by a relative error of at most 0.023.
Values may be sent and summed in bfloat16 or wider, within the bound.
A program may use at most 128 MiB of HBM per device.

```python
import math
import jax
import jax.numpy as jnp
import numpy as np
from jax import lax

D = 2048
HEAD = 64
HQ = 32
KVH = 16
FF = 2048
WINDOW = 128
TOP = 2
SEQ = 4096
TOKENS = 4096
TOK_DEV = 128
EXPERTS = 4
CAP = 80
N_SP = 4
N_TP = 8


def drawn_keys(key):
    base = jnp.clip(jax.random.normal(jax.random.fold_in(key, 101), (SEQ, KVH * HEAD), jnp.float32), -6.0, 6.0)
    return base


def draw_key_heads(key, part):
    base = drawn_keys(key)
    return base.astype(jnp.bfloat16)


def draw_query_heads(key, part):
    queries = jnp.clip(jax.random.normal(jax.random.fold_in(key, 104), (SEQ, HQ * HEAD), jnp.float32), -6.0, 6.0)
    return queries.astype(jnp.bfloat16)


def steps_of(key, extent, shards, least, top_value):
    factor_of, own = 1.0, jax.random.fold_in(key, 6)
    for axis_at, blocks in shards:
        draws = jnp.exp(jax.random.uniform(jax.random.fold_in(own, axis_at), (blocks,), jnp.float32, least / len(shards), top_value / len(shards)))
        factor_of = factor_of * jnp.repeat(draws, extent[axis_at] // blocks).reshape([-1 if axis == axis_at else 1 for axis in range(len(extent))])
    return factor_of


def routed_block(stream_key, own, number, rows, amount, top, limit, slope):
    order = jax.random.permutation(stream_key, amount)
    packed, common = shares(amount, rows * top, limit, slope, True), shares(amount, rows * top, limit, slope, False)
    places = jnp.arange(amount)

    def named(lengths, offset_by):
        used = int((lengths > 0).sum())
        fixed = max(1, used // 4)
        shifted = fixed + (places - fixed + offset_by * (used - fixed)) % max(1, amount - fixed)
        return jnp.zeros((amount,), jnp.int32).at[order[jnp.where(places < fixed, places, shifted)]].set(jnp.asarray(lengths, jnp.int32))

    lengths = jnp.where(number % 4 == 0, named(packed, number // 4), named(common, number - number // 4 - 1))
    mixed = jax.random.permutation(jax.random.fold_in(own, 3), amount)
    donor, sink = mixed[0:amount // 2 * 2:2], mixed[1:amount // 2 * 2:2]
    room = jnp.minimum(lengths[donor] - 1, limit - lengths[sink]) // 2
    room = jnp.where((donor == order[0]) | (sink == order[0]) | (lengths[sink] == 0), 0, jnp.maximum(room, 0))
    shifted = jax.random.randint(jax.random.fold_in(own, 4), (amount // 2,), 0, 1 << 20) % (room + 1)
    lengths = lengths.at[donor].add(-shifted).at[sink].add(shifted)
    members = jnp.searchsorted(jnp.cumsum(lengths), jnp.arange(rows * top), side="right").astype(jnp.int32)
    grid = members.reshape(top, rows).T
    grid = grid[jax.random.permutation(jax.random.fold_in(own, 1), rows)]
    offset_by = jax.random.randint(jax.random.fold_in(own, 2), (rows, 1), 0, top)
    return jnp.take_along_axis(grid, (jnp.arange(top)[None, :] + offset_by) % top, axis=1)


def shares(amount, total, bound, slope, full):
    weights = [(1 << 20) // math.isqrt(standing ** slope) + 1 for standing in range(1, amount + 1)]
    largest = bound if full else min(bound, max(-(-total // amount), total * weights[0] // sum(weights)))
    least = 1 if total - largest >= amount - 1 else 0
    given, rest = [largest] + [least] * (amount - 1), total - largest - least * (amount - 1)
    while rest > 0:
        free = [i for i in range(1, amount) if given[i] < largest] or [i for i in range(1, amount) if given[i] < bound]
        pool, remaining = sum([weights[i] for i in free]), rest
        for i in free:
            extra = min(bound - given[i], max(1, remaining * weights[i] // pool), rest)
            given[i] = given[i] + extra
            rest = rest - extra
    return np.array(given)


def centred(own_key, dims, spread, limit, shards=(), held_as=jnp.bfloat16):
    array = spread * jax.random.normal(own_key, dims, jnp.float32)
    if shards:
        array = array * steps_of(own_key, dims, shards, -0.22, 0.18)
    return jnp.clip(array, -limit, limit).astype(held_as)


def setup_inputs(seed: int = 0) -> dict:
    arg_keys = jax.random.split(jax.random.key(seed), 13)
    query_heads = draw_query_heads(jax.random.fold_in(arg_keys[12], 71), 0)
    key_heads = draw_key_heads(jax.random.fold_in(arg_keys[12], 71), 0)
    value_heads = centred(arg_keys[2], (SEQ, KVH * HEAD), 1.0, 6.0, ((0, 4), (1, 8)))
    sink_logit = jnp.clip(3.0 + 4.0 * jax.random.uniform(arg_keys[3], (HQ,), jnp.float32) ** steps_of(arg_keys[3], (HQ,), ((0, 8),), -0.2, 0.2), 3.0, 7.0)
    residual = centred(arg_keys[4], (TOKENS, D), 1.0, 6.0, ((0, 32),))
    out_weight = centred(arg_keys[5], (HQ * HEAD, D), (HQ * HEAD // 16) ** -0.5, 0.5)
    norm_gain = jnp.clip(1.0 + 0.18 * jax.random.normal(arg_keys[6], (D,), jnp.float32), 0.1, 1.9)
    routes_keys = jax.random.split(jax.random.fold_in(arg_keys[7], 1), TOKENS // TOK_DEV)
    routes_turns = jax.random.permutation(jax.random.fold_in(arg_keys[7], 3), TOKENS // TOK_DEV)
    routes = jax.vmap(lambda own, number: routed_block(jax.random.fold_in(arg_keys[7], 2), own, number, TOK_DEV, EXPERTS, TOP, CAP, 1))(routes_keys, routes_turns).reshape((TOKENS, TOP))
    route_weight = jnp.clip(0.2 + 0.8 * jax.random.uniform(arg_keys[8], (TOKENS, TOP), jnp.float32) ** steps_of(arg_keys[8], (TOKENS, TOP), ((0, 32),), -0.2, 0.2), 0.2, 1.0)
    gate_weight = centred(arg_keys[9], (EXPERTS, D, FF), (D // 6) ** -0.5, 0.3125, ((0, 4), (2, 8)))
    up_weight = centred(arg_keys[10], (EXPERTS, D, FF), (D // 6) ** -0.5, 0.3125, ((0, 4), (2, 8)))
    down_weight = centred(arg_keys[11], (EXPERTS, FF, D), (FF * 4) ** -0.5, 0.0625, ((0, 4), (1, 8)))
    return {"query_heads": query_heads, "key_heads": key_heads, "value_heads": value_heads, "sink_logit": sink_logit, "residual": residual, "out_weight": out_weight, "norm_gain": norm_gain, "routes": routes, "route_weight": route_weight, "gate_weight": gate_weight, "up_weight": up_weight, "down_weight": down_weight}


eps = 1e-06
clamp_limit = 7.0
sigmoid_alpha = 1.702

def attention(query_heads, key_heads, value_heads, sink_logit):
    block_count = TOKENS // WINDOW
    group_size = HQ // KVH
    queries = query_heads.reshape(block_count, WINDOW, KVH, group_size, HEAD).transpose(2, 0, 1, 3, 4)
    key_blocks = key_heads.reshape(block_count, WINDOW, KVH, HEAD).transpose(2, 0, 1, 3)
    value_blocks = value_heads.reshape(block_count, WINDOW, KVH, HEAD).transpose(2, 0, 1, 3)
    sinks = sink_logit.reshape(KVH, group_size)
    query_pos = jnp.arange(WINDOW)[:, None]
    key_col = jnp.arange(2 * WINDOW)[None, :]
    distance = query_pos + WINDOW - key_col
    block_ids = jnp.arange(block_count)[:, None, None]
    key_global = (block_ids - 1) * WINDOW + key_col[None]
    allowed = (distance[None] >= 0) & (distance[None] < WINDOW) & (key_global >= 0)

    def banded(current):
        earlier = jnp.concatenate([jnp.zeros_like(current[:1]), current[:-1]], axis=0)
        return jnp.concatenate([earlier, current], axis=1)

    def one_head(items):
        query_part, key_part, value_part, sink_part = items
        key_band = banded(key_part).astype(jnp.float32)
        value_band = banded(value_part).astype(jnp.float32)
        scores = jnp.einsum('nqgd,nkd->ngqk', query_part.astype(jnp.float32), key_band) * HEAD ** (-0.5)
        logits = jnp.where(allowed[:, None], scores, -jnp.inf)
        sink_term = sink_part[None, :, None, None]
        row_max = jnp.maximum(lax.optimization_barrier(jnp.max(logits, axis=-1, keepdims=True)), sink_term)
        raised = jnp.exp(logits - row_max)
        weights_bf = (raised / (lax.optimization_barrier(jnp.sum(raised, axis=-1, keepdims=True)) + jnp.exp(sink_term - row_max))).astype(jnp.bfloat16)
        result = jnp.einsum('ngqk,nkd->nqgd', weights_bf.astype(jnp.float32), value_band)
        return result.astype(jnp.bfloat16)
    heads_out = lax.map(one_head, (queries, key_blocks, value_blocks, sinks))
    return heads_out.transpose(1, 2, 0, 3, 4).reshape(TOKENS, HQ * HEAD)

def reference(query_heads, key_heads, value_heads, sink_logit, residual, out_weight, norm_gain, routes, route_weight, gate_weight, up_weight, down_weight):
    attended = attention(query_heads, key_heads, value_heads, sink_logit)
    mixed = jnp.dot(attended, out_weight, preferred_element_type=jnp.float32)
    stream = (residual.astype(jnp.float32) + mixed).astype(jnp.bfloat16)
    stream32 = stream.astype(jnp.float32)
    normed = (stream32 * lax.rsqrt(lax.optimization_barrier(jnp.mean(stream32 * stream32, axis=-1, keepdims=True)) + eps) * norm_gain).astype(jnp.bfloat16)
    device_count = N_SP * N_TP
    choice_rows = routes.reshape(device_count, TOK_DEV * TOP)
    one_hot = (choice_rows[:, :, None] == jnp.arange(EXPERTS, dtype=jnp.int32)[None, None, :]).astype(jnp.int32)
    ranked = lax.optimization_barrier(jnp.sum((jnp.cumsum(one_hot, axis=1) - one_hot) * one_hot, axis=-1)).astype(jnp.int32)
    device_ids = jnp.arange(device_count, dtype=jnp.int32)[:, None]
    token_ids = device_ids * TOK_DEV + jnp.arange(TOK_DEV * TOP, dtype=jnp.int32)[None, :] // TOP
    table = jnp.full((device_count, EXPERTS, CAP), TOKENS, dtype=jnp.int32)
    table = table.at[device_ids, choice_rows, ranked].set(token_ids.astype(jnp.int32))
    padded = jnp.concatenate([normed, jnp.zeros((1, D), jnp.bfloat16)], axis=0)

    def run_expert(index):
        row_block = padded[table[:, index, :].reshape(-1)]
        gate_pre = jnp.dot(row_block, gate_weight[index], preferred_element_type=jnp.float32)
        upward = jnp.dot(row_block, up_weight[index], preferred_element_type=jnp.float32)
        capped = jnp.minimum(gate_pre, clamp_limit)
        linear = jnp.clip(upward, -clamp_limit, clamp_limit)
        hidden = (capped * jax.nn.sigmoid(sigmoid_alpha * capped) * (linear + 1.0)).astype(jnp.bfloat16)
        pieces = hidden.astype(jnp.float32).reshape(device_count * CAP, N_TP, FF // N_TP)
        down_pieces = down_weight[index].astype(jnp.float32).reshape(N_TP, FF // N_TP, D)
        partial_value = jnp.einsum('rjf,jfd->jrd', pieces, down_pieces).astype(jnp.bfloat16)
        return lax.optimization_barrier(jnp.sum(partial_value.astype(jnp.float32), axis=0)).astype(jnp.bfloat16)
    outputs = lax.map(run_expert, jnp.arange(EXPERTS, dtype=jnp.int32))
    shaped = outputs.reshape(EXPERTS, device_count, CAP, D)
    picked = shaped[choice_rows, device_ids, ranked]
    combined = lax.optimization_barrier(jnp.sum(picked.astype(jnp.float32).reshape(TOKENS, TOP, D) * route_weight[:, :, None], axis=1))
    return (stream32 + combined).astype(jnp.bfloat16)
```

```python
import functools

import jax
import jax.numpy as jnp
from jax import lax
from jax.experimental import pallas as pl
from jax.experimental.pallas import tpu as pltpu
from jax.sharding import PartitionSpec as P

HEAD = 64
WINDOW = 128


eps = 1e-06
clamp_limit = 7.0
sigmoid_alpha = 1.702


def from_behind(block, axis, distance):
    devices = range(lax.axis_size(axis))
    route = [(i - distance, i) for i in devices if i - distance in devices]
    return lax.ppermute(block, axis, route)


MESH = pl.DeviceIdType.MESH
CORES = 2


def round_up(value, unit):
    return (value + unit - 1) // unit * unit


def place():
    tp = lax.axis_index("tp")
    return lax.axis_index("sp"), tp // CORES, lax.rem(tp, CORES)


def partner_of(sp, d, n_sp):
    if n_sp & (n_sp - 1):
        return lax.rem(sp + d, n_sp)
    total, bit = 0, 1
    while bit < n_sp:
        total = total + lax.rem(sp // bit + d // bit, 2) * bit
        bit *= 2
    return total


def source_of(sp, d, n_sp):
    if n_sp & (n_sp - 1):
        return lax.rem(sp + n_sp - d, n_sp)
    return partner_of(sp, d, n_sp)


def greet(n_sp, nz, sp, z, c):
    barrier = pltpu.get_barrier_semaphore()
    tp = z * CORES + c
    for d in range(1, n_sp):
        pl.semaphore_signal(
            barrier, inc=1, device_id=(partner_of(sp, d, n_sp), tp), device_id_type=MESH
        )
    pl.semaphore_signal(
        barrier, inc=1, device_id=(sp, z * CORES + 1 - c), device_id_type=MESH
    )

    @pl.when(z > 0)
    def _():
        pl.semaphore_signal(barrier, inc=1, device_id=(sp, tp - CORES), device_id_type=MESH)

    @pl.when(z < nz - 1)
    def _():
        pl.semaphore_signal(barrier, inc=1, device_id=(sp, tp + CORES), device_id_type=MESH)

    beside = jnp.where(z > 0, 1, 0) + jnp.where(z < nz - 1, 1, 0)
    pl.semaphore_wait(barrier, n_sp + beside)


def send(src, dst, send_sem, recv_sem, device):
    return pltpu.make_async_remote_copy(
        src_ref=src,
        dst_ref=dst,
        send_sem=send_sem,
        recv_sem=recv_sem,
        device_id=device,
        device_id_type=MESH,
    )


def nearest_first(z, nz, visit):
    def step(j, carry):
        away = j // 2 + 1
        behind = lax.rem(j, 2)
        block = z + away * (1 - 2 * behind)

        @pl.when((block >= 0) & (block < nz))
        def _():
            visit(block, behind)

        return carry

    lax.fori_loop(0, 2 * (nz - 1), step, 0)


def farthest_first(z, nz, visit):
    def step(j, carry):
        away = nz - 1 - j // 2
        behind = lax.rem(j, 2)
        block = z + away * (1 - 2 * behind)

        @pl.when((block >= 0) & (block < nz))
        def _():
            visit(block, behind)

        return carry

    lax.fori_loop(0, 2 * (nz - 1), step, 0)


def dispatch_kernel(
    n_sp, nz, normed, onehot, gate, up, hid, toks, comp, rows,
    up_s, up_r, dn_s, dn_r, x_s, x_r, p_s, p_r,
):
    sp, z, c = place()
    tp = z * CORES + c
    peer_core = (sp, z * CORES + 1 - c)
    above = (sp, lax.rem(z + 1, nz) * CORES + c)
    below = (sp, lax.rem(z + nz - 1, nz) * CORES + c)
    capp, width = comp.shape[2], comp.shape[3]
    greet(n_sp, nz, sp, z, c)

    def to_above(block, src):
        return send(src, toks.at[block], up_s.at[block], up_r.at[block], above)

    def to_below(block, src):
        return send(src, toks.at[block], dn_s.at[block], dn_r.at[block], below)

    def to_expert(block, d):
        e = partner_of(sp, d, n_sp)
        return send(
            comp.at[block, e], rows.at[block, c, sp],
            x_s.at[block, d], x_r.at[block, d], (e, tp),
        )

    def from_expert(block, d):
        e = source_of(sp, d, n_sp)
        return send(
            comp.at[block, e], rows.at[block, c, e],
            x_s.at[block, d], x_r.at[block, d], (e, tp),
        )

    def to_core(block, d):
        e = source_of(sp, d, n_sp)
        return send(
            rows.at[block, c, e], rows.at[block, c, e],
            p_s.at[block, d], p_r.at[block, d], peer_core,
        )

    def from_core(block, d):
        e = source_of(sp, d, n_sp)
        return send(
            rows.at[block, 1 - c, e], rows.at[block, 1 - c, e],
            p_s.at[block, d], p_r.at[block, d], peer_core,
        )

    def own_to_core(block):
        return send(
            comp.at[block, sp], rows.at[block, c, sp],
            p_s.at[block, 0], p_r.at[block, 0], peer_core,
        )

    def deal(block, src):
        def one(e, carry):
            comp[block, e] = jnp.dot(
                onehot[block, pl.ds(pl.multiple_of(e * capp, capp), capp), :],
                src[...],
                preferred_element_type=jnp.float32,
            ).astype(jnp.bfloat16)
            return carry

        lax.fori_loop(0, n_sp, one, 0)
        for d in range(1, n_sp):
            to_expert(block, d).start()
        own_to_core(block).start()
        rows[block, c, sp] = comp[block, sp]

    @pl.when(z < nz - 1)
    def _():
        to_above(z, normed).start()

    @pl.when(z > 0)
    def _():
        to_below(z, normed).start()

    deal(z, normed)

    def gather(block, behind):
        @pl.when(behind == 1)
        def _():
            to_above(block, toks.at[block]).wait_recv()

            @pl.when(z < nz - 1)
            def _():
                to_above(block, toks.at[block]).start()

        @pl.when(behind == 0)
        def _():
            to_below(block, toks.at[block]).wait_recv()

            @pl.when(z > 0)
            def _():
                to_below(block, toks.at[block]).start()

        deal(block, toks.at[block])

    nearest_first(z, nz, gather)

    def units(block, lane):
        tile = rows[block, lane].reshape(n_sp * capp, width)
        gate_pre = jnp.dot(tile, gate[...], preferred_element_type=jnp.float32)
        upward = jnp.dot(tile, up[...], preferred_element_type=jnp.float32)
        capped = jnp.minimum(gate_pre, clamp_limit)
        linear = jnp.clip(upward, -clamp_limit, clamp_limit)
        gated = capped * jax.nn.sigmoid(sigmoid_alpha * capped)
        hid[block, lane] = (gated * (linear + 1.0)).astype(jnp.bfloat16)

    def serve(block, behind):
        for d in range(1, n_sp):
            from_expert(block, d).wait_recv()
            to_core(block, d).start()

        def both(i, carry):
            @pl.when(i == 1)
            def _():
                for d in range(n_sp):
                    from_core(block, d).wait_recv()

            units(block, lax.rem(c + i, CORES))
            return carry

        lax.fori_loop(0, CORES, both, 0)
        for d in range(1, n_sp):
            to_expert(block, d).wait_send()
            to_core(block, d).wait_send()
        own_to_core(block).wait_send()

    serve(z, 0)
    nearest_first(z, nz, serve)

    @pl.when(z < nz - 1)
    def _():
        to_above(z, normed).wait_send()

    @pl.when(z > 0)
    def _():
        to_below(z, normed).wait_send()

    def drain(block, behind):
        @pl.when((behind == 1) & (z < nz - 1))
        def _():
            to_above(block, toks.at[block]).wait_send()

        @pl.when((behind == 0) & (z > 0))
        def _():
            to_below(block, toks.at[block]).wait_send()

    nearest_first(z, nz, drain)


def return_kernel(
    n_sp, nz, tile_cols, hid, down, share_hi, share_lo, stream, out,
    p_out, p_in, sums, back, a_out, a_up, a_dn,
    up_s, up_r, dn_s, dn_r, x_s, x_r, p_s, p_r,
):
    sp, z, c = place()
    tp = z * CORES + c
    peer_core = (sp, z * CORES + 1 - c)
    above = (sp, lax.rem(z + 1, nz) * CORES + c)
    below = (sp, lax.rem(z + nz - 1, nz) * CORES + c)
    capp, width = sums.shape[2], sums.shape[3]
    col_tiles = width // tile_cols
    greet(n_sp, nz, sp, z, c)

    def cols_of(t):
        return pl.ds(pl.multiple_of(t * tile_cols, tile_cols), tile_cols)

    def to_core(block):
        return send(p_out.at[block], p_in.at[block], p_s.at[block], p_r.at[block], peer_core)

    def to_home(block, d):
        e = partner_of(sp, d, n_sp)
        return send(
            sums.at[block, e], back.at[block, sp],
            x_s.at[block, d], x_r.at[block, d], (e, tp),
        )

    def from_home(block, d):
        e = source_of(sp, d, n_sp)
        return send(
            sums.at[block, e], back.at[block, e],
            x_s.at[block, d], x_r.at[block, d], (e, tp),
        )

    def to_above(block):
        return send(a_out.at[block], a_up.at[block], up_s.at[block], up_r.at[block], above)

    def to_below(block):
        return send(a_out.at[block], a_dn.at[block], dn_s.at[block], dn_r.at[block], below)

    def lend(block, behind):
        def one(t, carry):
            cols = cols_of(t)
            p_out[block, :, cols] = jnp.dot(
                hid[block, 1 - c], down[:, cols], preferred_element_type=jnp.float32
            ).astype(jnp.bfloat16)
            return carry

        lax.fori_loop(0, col_tiles, one, 0)
        to_core(block).start()

    def push(block, behind):
        to_core(block).wait_recv()

        def one(t, carry):
            cols = cols_of(t)
            part = jnp.dot(hid[block, c], down[:, cols], preferred_element_type=jnp.float32)
            both = (part + p_in[block, :, cols].astype(jnp.float32)).astype(jnp.bfloat16)
            sums[block, :, :, cols] = both.reshape(n_sp, capp, tile_cols)
            return carry

        lax.fori_loop(0, col_tiles, one, 0)
        for d in range(1, n_sp):
            to_home(block, d).start()
        back[block, sp] = sums[block, sp]

    def combined(block, cols):
        picked = back[block, :, :, cols].reshape(n_sp * capp, tile_cols)
        return jnp.dot(share_hi[block], picked, preferred_element_type=jnp.float32) + jnp.dot(
            share_lo[block], picked, preferred_element_type=jnp.float32
        )

    def await_home(block):
        for d in range(1, n_sp):
            from_home(block, d).wait_recv()

    def relay(block, behind):
        await_home(block)

        @pl.when(behind == 0)
        def _():
            @pl.when(z > 0)
            def _():
                to_above(block).wait_recv()

            def one(t, carry):
                cols = cols_of(t)
                total = combined(block, cols)
                total = jnp.where(z > 0, total + a_up[block, :, cols].astype(jnp.float32), total)
                a_out[block, :, cols] = total.astype(jnp.bfloat16)
                return carry

            lax.fori_loop(0, col_tiles, one, 0)
            to_above(block).start()

        @pl.when(behind == 1)
        def _():
            @pl.when(z < nz - 1)
            def _():
                to_below(block).wait_recv()

            def one(t, carry):
                cols = cols_of(t)
                total = combined(block, cols)
                total = jnp.where(
                    z < nz - 1, total + a_dn[block, :, cols].astype(jnp.float32), total
                )
                a_out[block, :, cols] = total.astype(jnp.bfloat16)
                return carry

            lax.fori_loop(0, col_tiles, one, 0)
            to_below(block).start()

    farthest_first(z, nz, lend)
    lend(z, 0)
    farthest_first(z, nz, push)
    push(z, 0)
    farthest_first(z, nz, relay)
    await_home(z)

    @pl.when(z > 0)
    def _():
        to_above(z).wait_recv()

    @pl.when(z < nz - 1)
    def _():
        to_below(z).wait_recv()

    def final(t, carry):
        cols = cols_of(t)
        total = combined(z, cols)
        total = jnp.where(z > 0, total + a_up[z, :, cols].astype(jnp.float32), total)
        total = jnp.where(z < nz - 1, total + a_dn[z, :, cols].astype(jnp.float32), total)
        out[:, cols] = (stream[:, cols].astype(jnp.float32) + total).astype(jnp.bfloat16)
        return carry

    lax.fori_loop(0, col_tiles, final, 0)

    def drain(block, behind):
        to_core(block).wait_send()
        for d in range(1, n_sp):
            to_home(block, d).wait_send()

    def drain_line(block, behind):
        drain(block, behind)

        @pl.when(behind == 0)
        def _():
            to_above(block).wait_send()

        @pl.when(behind == 1)
        def _():
            to_below(block).wait_send()

    drain(z, 0)
    farthest_first(z, nz, drain_line)


def experts(normed, stream, routes, route_weight, gate_local, up_local, down_local, capacity):
    n_sp = lax.axis_size("sp")
    n_tp = lax.axis_size("tp")
    nz = n_tp // CORES
    tok, width = normed.shape
    units = gate_local.shape[1]
    choose = routes.shape[1]
    capp = round_up(capacity, 16)
    slots = n_sp * capp
    core = lax.rem(lax.axis_index("tp"), CORES)
    lane_routes = lax.dynamic_index_in_dim(
        routes.reshape(nz, CORES, tok, choose), core, 1, keepdims=False
    )
    ids = lane_routes.transpose(0, 2, 1)
    named = (ids[:, :, None, :] == jnp.arange(n_sp, dtype=jnp.int32)[None, None, :, None])
    member = jnp.any(named, axis=1)
    earlier = jnp.arange(tok)[:, None] < jnp.arange(tok)[None, :]
    rank = jnp.einsum(
        "zet,tu->zeu",
        member.astype(jnp.bfloat16),
        earlier.astype(jnp.bfloat16),
        preferred_element_type=jnp.float32,
    )
    own_rank = jnp.sum(jnp.where(named, rank[:, None], 0.0), axis=2).astype(jnp.int32)
    slot = ids * capp + own_rank
    places = jnp.arange(slots, dtype=jnp.int32)
    onehot = jnp.any(slot[:, :, None, :] == places[None, None, :, None], axis=1).astype(jnp.bfloat16)
    all_weight = lax.all_gather(route_weight, "tp", axis=0, tiled=False)
    lane_weight = lax.dynamic_index_in_dim(
        all_weight.reshape(nz, CORES, tok, choose), core, 1, keepdims=False
    )
    slot_t = slot.transpose(0, 2, 1)
    share = jnp.sum(
        jnp.where(
            slot_t[:, :, :, None] == places[None, None, None, :], lane_weight[:, :, :, None], 0.0
        ),
        axis=2,
    )
    share_hi = share.astype(jnp.bfloat16)
    share_lo = (share - share_hi.astype(jnp.float32)).astype(jnp.bfloat16)
    vmem = pl.BlockSpec(memory_space=pltpu.VMEM)
    dma = pltpu.SemaphoreType.DMA
    bf = jnp.bfloat16
    line = [dma((nz,))] * 4
    hid = pl.pallas_call(
        functools.partial(dispatch_kernel, n_sp, nz),
        out_shape=jax.ShapeDtypeStruct((nz, CORES, slots, units), bf),
        in_specs=[vmem] * 4,
        out_specs=vmem,
        scratch_shapes=[
            pltpu.VMEM((nz, tok, width), bf),
            pltpu.VMEM((nz, n_sp, capp, width), bf),
            pltpu.VMEM((nz, CORES, n_sp, capp, width), bf),
        ]
        + line
        + [dma((nz, n_sp))] * 4,
        compiler_params=pltpu.CompilerParams(
            collective_id=0, has_side_effects=True, vmem_limit_bytes=58 * 1024 * 1024
        ),
        name="dispatch",
    )(normed, onehot, gate_local, up_local)
    return pl.pallas_call(
        functools.partial(return_kernel, n_sp, nz, min(512, width)),
        out_shape=jax.ShapeDtypeStruct((tok, width), bf),
        in_specs=[vmem] * 5,
        out_specs=vmem,
        scratch_shapes=[
            pltpu.VMEM((nz, slots, width), bf),
            pltpu.VMEM((nz, slots, width), bf),
            pltpu.VMEM((nz, n_sp, capp, width), bf),
            pltpu.VMEM((nz, n_sp, capp, width), bf),
            pltpu.VMEM((nz, tok, width), bf),
            pltpu.VMEM((nz, tok, width), bf),
            pltpu.VMEM((nz, tok, width), bf),
        ]
        + line
        + [dma((nz, n_sp))] * 2
        + [dma((nz,))] * 2,
        compiler_params=pltpu.CompilerParams(
            collective_id=1, has_side_effects=True, vmem_limit_bytes=62 * 1024 * 1024
        ),
        name="give_back",
    )(hid, down_local, share_hi, share_lo, stream)


def local(
    query_heads,
    key_heads,
    value_heads,
    sink_logit,
    residual,
    out_weight,
    norm_gain,
    routes,
    route_weight,
    gate_weight,
    up_weight,
    down_weight,
):
    sp_count = lax.axis_size("sp")
    span_rows = query_heads.shape[0]
    kv_local = key_heads.shape[1] // HEAD
    group_size = query_heads.shape[1] // key_heads.shape[1]
    block_count = span_rows // WINDOW
    key_tail, value_tail = from_behind(
        (key_heads[span_rows - WINDOW :], value_heads[span_rows - WINDOW :]), "sp", 1
    )

    def banded(current, tail):
        shaped = current.reshape(block_count, WINDOW, kv_local, HEAD)
        earlier = jnp.concatenate([tail.reshape(1, WINDOW, kv_local, HEAD), shaped[:-1]], axis=0)
        return jnp.concatenate([earlier, shaped], axis=1)

    key_band = banded(key_heads, key_tail)
    value_band = banded(value_heads, value_tail)
    query_blocks = query_heads.reshape(block_count, WINDOW, kv_local, group_size, HEAD)
    scores = jnp.einsum(
        "nqhgd,nkhd->nhgqk", query_blocks, key_band, preferred_element_type=jnp.float32
    ) * HEAD ** (-0.5)
    query_pos = jnp.arange(WINDOW)[:, None]
    key_col = jnp.arange(2 * WINDOW)[None, :]
    distance = query_pos + WINDOW - key_col
    block_ids = jnp.arange(block_count)[:, None, None]
    key_global = lax.axis_index("sp") * span_rows + (block_ids - 1) * WINDOW + key_col[None]
    allowed = (distance[None] >= 0) & (distance[None] < WINDOW) & (key_global >= 0)
    logits = jnp.where(allowed[:, None, None], scores, -jnp.inf)
    sink_term = sink_logit.reshape(kv_local, group_size)[None, :, :, None, None]
    row_max = jnp.maximum(jnp.max(logits, axis=-1, keepdims=True), sink_term)
    raised = jnp.exp(logits - row_max)
    weights_bf = (
        raised / (jnp.sum(raised, axis=-1, keepdims=True) + jnp.exp(sink_term - row_max))
    ).astype(jnp.bfloat16)
    attended = jnp.einsum(
        "nhgqk,nkhd->nqhgd", weights_bf, value_band, preferred_element_type=jnp.float32
    )
    attended = attended.astype(jnp.bfloat16).reshape(span_rows, query_heads.shape[1])
    tok_rows = residual.shape[0]
    tp_index = lax.axis_index("tp")
    token_heads = lax.all_to_all(attended, "tp", split_axis=0, concat_axis=1, tiled=True)
    mixed = jnp.dot(token_heads, out_weight, preferred_element_type=jnp.float32)
    stream = (residual.astype(jnp.float32) + mixed).astype(jnp.bfloat16)
    stream32 = stream.astype(jnp.float32)
    normed = (
        stream32
        * lax.rsqrt(jnp.mean(stream32 * stream32, axis=-1, keepdims=True) + eps)
        * norm_gain
    ).astype(jnp.bfloat16)
    choose_count = routes.shape[1]
    capacity = max(2, 5 * tok_rows * choose_count // (4 * sp_count))
    return experts(
        normed, stream, routes, route_weight, gate_weight[0], up_weight[0], down_weight[0], capacity
    )


def solution(mesh):
    placed = (
        P("sp", "tp"),
        P("sp", "tp"),
        P("sp", "tp"),
        P("tp"),
        P(("sp", "tp"), None),
        P(),
        P(),
        P("sp", None),
        P(("sp", "tp"), None),
        P("sp", None, "tp"),
        P("sp", None, "tp"),
        P("sp", "tp", None),
    )
    return jax.shard_map(
        local, mesh=mesh, in_specs=placed, out_specs=P(("sp", "tp"), None), check_vma=False
    )
```

```python
import functools

import jax
import jax.numpy as jnp
from jax import lax
from jax.experimental import pallas as pl
from jax.experimental.pallas import tpu as pltpu
from jax.sharding import PartitionSpec as P

HEAD = 64
WINDOW = 128


eps = 1e-06
clamp_limit = 7.0
sigmoid_alpha = 1.702


MESH = pl.DeviceIdType.MESH
CORES = 2
LANES = 128


def round_up(value, unit):
    return (value + unit - 1) // unit * unit


def place():
    tp = lax.axis_index("tp")
    return lax.axis_index("sp"), tp // CORES, lax.rem(tp, CORES)


def partner_of(sp, d, n_sp):
    if n_sp & (n_sp - 1):
        return lax.rem(sp + d, n_sp)
    total, bit = 0, 1
    while bit < n_sp:
        total = total + lax.rem(sp // bit + d // bit, 2) * bit
        bit *= 2
    return total


def source_of(sp, d, n_sp):
    if n_sp & (n_sp - 1):
        return lax.rem(sp + n_sp - d, n_sp)
    return partner_of(sp, d, n_sp)


def greet(n_sp, nz, sp, z, c):
    barrier = pltpu.get_barrier_semaphore()
    tp = z * CORES + c
    for d in range(1, n_sp):
        pl.semaphore_signal(
            barrier, inc=1, device_id=(partner_of(sp, d, n_sp), tp), device_id_type=MESH
        )
    pl.semaphore_signal(
        barrier, inc=1, device_id=(sp, z * CORES + 1 - c), device_id_type=MESH
    )

    @pl.when(z > 0)
    def _():
        pl.semaphore_signal(barrier, inc=1, device_id=(sp, tp - CORES), device_id_type=MESH)

    @pl.when(z < nz - 1)
    def _():
        pl.semaphore_signal(barrier, inc=1, device_id=(sp, tp + CORES), device_id_type=MESH)

    beside = jnp.where(z > 0, 1, 0) + jnp.where(z < nz - 1, 1, 0)
    pl.semaphore_wait(barrier, n_sp + beside)


def send(src, dst, send_sem, recv_sem, device):
    return pltpu.make_async_remote_copy(
        src_ref=src,
        dst_ref=dst,
        send_sem=send_sem,
        recv_sem=recv_sem,
        device_id=device,
        device_id_type=MESH,
    )


def nearest_first(z, nz, visit):
    def step(j, carry):
        away = j // 2 + 1
        behind = lax.rem(j, 2)
        block = z + away * (1 - 2 * behind)

        @pl.when((block >= 0) & (block < nz))
        def _():
            visit(block, behind)

        return carry

    lax.fori_loop(0, 2 * (nz - 1), step, 0)


def farthest_first(z, nz, visit):
    def step(j, carry):
        away = nz - 1 - j // 2
        behind = lax.rem(j, 2)
        block = z + away * (1 - 2 * behind)

        @pl.when((block >= 0) & (block < nz))
        def _():
            visit(block, behind)

        return carry

    lax.fori_loop(0, 2 * (nz - 1), step, 0)


def dispatch_kernel(
    n_sp, nz, normed, onehot, gate, up, hid, shares, toks, comp, rows,
    up_s, up_r, dn_s, dn_r, x_s, x_r, p_s, p_r,
):
    sp, z, c = place()
    tp = z * CORES + c
    peer_core = (sp, z * CORES + 1 - c)
    above = (sp, lax.rem(z + 1, nz) * CORES + c)
    below = (sp, lax.rem(z + nz - 1, nz) * CORES + c)
    capp, width = comp.shape[2], comp.shape[3]
    greet(n_sp, nz, sp, z, c)

    def to_above(block, src):
        return send(src, toks.at[block], up_s.at[block], up_r.at[block], above)

    def to_below(block, src):
        return send(src, toks.at[block], dn_s.at[block], dn_r.at[block], below)

    def to_expert(block, d):
        e = partner_of(sp, d, n_sp)
        return send(
            comp.at[block, e], rows.at[block, c, sp],
            x_s.at[block, d], x_r.at[block, d], (e, tp),
        )

    def from_expert(block, d):
        e = source_of(sp, d, n_sp)
        return send(
            comp.at[block, e], rows.at[block, c, e],
            x_s.at[block, d], x_r.at[block, d], (e, tp),
        )

    def to_core(block, d):
        e = source_of(sp, d, n_sp)
        return send(
            rows.at[block, c, e], rows.at[block, c, e],
            p_s.at[block, d], p_r.at[block, d], peer_core,
        )

    def from_core(block, d):
        e = source_of(sp, d, n_sp)
        return send(
            rows.at[block, 1 - c, e], rows.at[block, 1 - c, e],
            p_s.at[block, d], p_r.at[block, d], peer_core,
        )

    def own_to_core(block):
        return send(
            comp.at[block, sp], rows.at[block, c, sp],
            p_s.at[block, 0], p_r.at[block, 0], peer_core,
        )

    def deal(block, src):
        shares[block] = src[:, pl.ds(width, LANES)]

        def one(e, carry):
            comp[block, e] = jnp.dot(
                onehot[block, pl.ds(pl.multiple_of(e * capp, capp), capp), :],
                src[:, pl.ds(0, width)],
                preferred_element_type=jnp.float32,
            ).astype(jnp.bfloat16)
            return carry

        lax.fori_loop(0, n_sp, one, 0)
        for d in range(1, n_sp):
            to_expert(block, d).start()
        own_to_core(block).start()
        rows[block, c, sp] = comp[block, sp]

    @pl.when(z < nz - 1)
    def _():
        to_above(z, normed).start()

    @pl.when(z > 0)
    def _():
        to_below(z, normed).start()

    deal(z, normed)

    def gather(block, behind):
        @pl.when(behind == 1)
        def _():
            to_above(block, toks.at[block]).wait_recv()

            @pl.when(z < nz - 1)
            def _():
                to_above(block, toks.at[block]).start()

        @pl.when(behind == 0)
        def _():
            to_below(block, toks.at[block]).wait_recv()

            @pl.when(z > 0)
            def _():
                to_below(block, toks.at[block]).start()

        deal(block, toks.at[block])

    nearest_first(z, nz, gather)

    def units(block, lane):
        tile = rows[block, lane].reshape(n_sp * capp, width)
        gate_pre = jnp.dot(tile, gate[...], preferred_element_type=jnp.float32)
        upward = jnp.dot(tile, up[...], preferred_element_type=jnp.float32)
        capped = jnp.minimum(gate_pre, clamp_limit)
        linear = jnp.clip(upward, -clamp_limit, clamp_limit)
        gated = capped * jax.nn.sigmoid(sigmoid_alpha * capped)
        hid[block, lane] = (gated * (linear + 1.0)).astype(jnp.bfloat16)

    def serve(block, behind):
        for d in range(1, n_sp):
            from_expert(block, d).wait_recv()
            to_core(block, d).start()

        def both(i, carry):
            @pl.when(i == 1)
            def _():
                for d in range(n_sp):
                    from_core(block, d).wait_recv()

            units(block, lax.rem(c + i, CORES))
            return carry

        lax.fori_loop(0, CORES, both, 0)
        for d in range(1, n_sp):
            to_expert(block, d).wait_send()
            to_core(block, d).wait_send()
        own_to_core(block).wait_send()

    serve(z, 0)
    nearest_first(z, nz, serve)

    @pl.when(z < nz - 1)
    def _():
        to_above(z, normed).wait_send()

    @pl.when(z > 0)
    def _():
        to_below(z, normed).wait_send()

    def drain(block, behind):
        @pl.when((behind == 1) & (z < nz - 1))
        def _():
            to_above(block, toks.at[block]).wait_send()

        @pl.when((behind == 0) & (z > 0))
        def _():
            to_below(block, toks.at[block]).wait_send()

    nearest_first(z, nz, drain)


def return_kernel(
    n_sp, nz, tile_cols, hid, down, share_hi, share_lo, stream, out,
    p_out, p_in, sums, back, a_out, a_up, a_dn,
    up_s, up_r, dn_s, dn_r, x_s, x_r, p_s, p_r,
):
    sp, z, c = place()
    tp = z * CORES + c
    peer_core = (sp, z * CORES + 1 - c)
    above = (sp, lax.rem(z + 1, nz) * CORES + c)
    below = (sp, lax.rem(z + nz - 1, nz) * CORES + c)
    capp, width = sums.shape[2], sums.shape[3]
    col_tiles = width // tile_cols
    greet(n_sp, nz, sp, z, c)

    def cols_of(t):
        return pl.ds(pl.multiple_of(t * tile_cols, tile_cols), tile_cols)

    def to_core(block):
        return send(p_out.at[block], p_in.at[block], p_s.at[block], p_r.at[block], peer_core)

    def to_home(block, d):
        e = partner_of(sp, d, n_sp)
        return send(
            sums.at[block, e], back.at[block, sp],
            x_s.at[block, d], x_r.at[block, d], (e, tp),
        )

    def from_home(block, d):
        e = source_of(sp, d, n_sp)
        return send(
            sums.at[block, e], back.at[block, e],
            x_s.at[block, d], x_r.at[block, d], (e, tp),
        )

    def to_above(block):
        return send(a_out.at[block], a_up.at[block], up_s.at[block], up_r.at[block], above)

    def to_below(block):
        return send(a_out.at[block], a_dn.at[block], dn_s.at[block], dn_r.at[block], below)

    def lend(block, behind):
        def one(t, carry):
            cols = cols_of(t)
            p_out[block, :, cols] = jnp.dot(
                hid[block, 1 - c], down[:, cols], preferred_element_type=jnp.float32
            ).astype(jnp.bfloat16)
            return carry

        lax.fori_loop(0, col_tiles, one, 0)
        to_core(block).start()

    def push(block, behind):
        to_core(block).wait_recv()

        def one(t, carry):
            cols = cols_of(t)
            part = jnp.dot(hid[block, c], down[:, cols], preferred_element_type=jnp.float32)
            both = (part + p_in[block, :, cols].astype(jnp.float32)).astype(jnp.bfloat16)
            sums[block, :, :, cols] = both.reshape(n_sp, capp, tile_cols)
            return carry

        lax.fori_loop(0, col_tiles, one, 0)
        for d in range(1, n_sp):
            to_home(block, d).start()
        back[block, sp] = sums[block, sp]

    def combined(block, cols):
        picked = back[block, :, :, cols].reshape(n_sp * capp, tile_cols)
        return jnp.dot(share_hi[block], picked, preferred_element_type=jnp.float32) + jnp.dot(
            share_lo[block], picked, preferred_element_type=jnp.float32
        )

    def await_home(block):
        for d in range(1, n_sp):
            from_home(block, d).wait_recv()

    def relay(block, behind):
        await_home(block)

        @pl.when(behind == 0)
        def _():
            @pl.when(z > 0)
            def _():
                to_above(block).wait_recv()

            def one(t, carry):
                cols = cols_of(t)
                total = combined(block, cols)
                total = jnp.where(z > 0, total + a_up[block, :, cols].astype(jnp.float32), total)
                a_out[block, :, cols] = total.astype(jnp.bfloat16)
                return carry

            lax.fori_loop(0, col_tiles, one, 0)
            to_above(block).start()

        @pl.when(behind == 1)
        def _():
            @pl.when(z < nz - 1)
            def _():
                to_below(block).wait_recv()

            def one(t, carry):
                cols = cols_of(t)
                total = combined(block, cols)
                total = jnp.where(
                    z < nz - 1, total + a_dn[block, :, cols].astype(jnp.float32), total
                )
                a_out[block, :, cols] = total.astype(jnp.bfloat16)
                return carry

            lax.fori_loop(0, col_tiles, one, 0)
            to_below(block).start()

    farthest_first(z, nz, lend)
    lend(z, 0)
    farthest_first(z, nz, push)
    push(z, 0)
    farthest_first(z, nz, relay)
    await_home(z)

    @pl.when(z > 0)
    def _():
        to_above(z).wait_recv()

    @pl.when(z < nz - 1)
    def _():
        to_below(z).wait_recv()

    def final(t, carry):
        cols = cols_of(t)
        total = combined(z, cols)
        total = jnp.where(z > 0, total + a_up[z, :, cols].astype(jnp.float32), total)
        total = jnp.where(z < nz - 1, total + a_dn[z, :, cols].astype(jnp.float32), total)
        out[:, cols] = (stream[:, cols].astype(jnp.float32) + total).astype(jnp.bfloat16)
        return carry

    lax.fori_loop(0, col_tiles, final, 0)

    def drain(block, behind):
        to_core(block).wait_send()
        for d in range(1, n_sp):
            to_home(block, d).wait_send()

    def drain_line(block, behind):
        drain(block, behind)

        @pl.when(behind == 0)
        def _():
            to_above(block).wait_send()

        @pl.when(behind == 1)
        def _():
            to_below(block).wait_send()

    drain(z, 0)
    farthest_first(z, nz, drain_line)


def experts(normed, stream, routes, route_weight, gate_local, up_local, down_local, capacity):
    n_sp = lax.axis_size("sp")
    n_tp = lax.axis_size("tp")
    nz = n_tp // CORES
    tok, width = normed.shape
    units = gate_local.shape[1]
    choose = routes.shape[1]
    capp = round_up(capacity, 16)
    slots = n_sp * capp
    core = lax.rem(lax.axis_index("tp"), CORES)
    lane_routes = lax.dynamic_index_in_dim(
        routes.reshape(nz, CORES, tok, choose), core, 1, keepdims=False
    )
    ids = lane_routes.transpose(0, 2, 1)
    named = (ids[:, :, None, :] == jnp.arange(n_sp, dtype=jnp.int32)[None, None, :, None])
    member = jnp.any(named, axis=1)
    earlier = jnp.arange(tok)[:, None] < jnp.arange(tok)[None, :]
    rank = jnp.einsum(
        "zet,tu->zeu",
        member.astype(jnp.bfloat16),
        earlier.astype(jnp.bfloat16),
        preferred_element_type=jnp.float32,
    )
    own_rank = jnp.sum(jnp.where(named, rank[:, None], 0.0), axis=2).astype(jnp.int32)
    slot = ids * capp + own_rank
    places = jnp.arange(slots, dtype=jnp.int32)
    onehot = jnp.any(slot[:, :, None, :] == places[None, None, :, None], axis=1).astype(jnp.bfloat16)
    weight_hi = lax.reduce_precision(route_weight, 8, 7)
    weight_mid = lax.reduce_precision(route_weight - weight_hi, 8, 7)
    weight_lo = route_weight - weight_hi - weight_mid
    carried = jnp.concatenate([weight_hi, weight_mid, weight_lo], axis=1)
    carried = jnp.pad(carried, ((0, 0), (0, LANES - 3 * choose))).astype(jnp.bfloat16)
    payload = jnp.concatenate([normed, carried], axis=1)
    vmem = pl.BlockSpec(memory_space=pltpu.VMEM)
    dma = pltpu.SemaphoreType.DMA
    bf = jnp.bfloat16
    line = [dma((nz,))] * 4
    hid, shares = pl.pallas_call(
        functools.partial(dispatch_kernel, n_sp, nz),
        out_shape=(
            jax.ShapeDtypeStruct((nz, CORES, slots, units), bf),
            jax.ShapeDtypeStruct((nz, tok, LANES), bf),
        ),
        in_specs=[vmem] * 4,
        out_specs=(vmem, vmem),
        scratch_shapes=[
            pltpu.VMEM((nz, tok, width + LANES), bf),
            pltpu.VMEM((nz, n_sp, capp, width), bf),
            pltpu.VMEM((nz, CORES, n_sp, capp, width), bf),
        ]
        + line
        + [dma((nz, n_sp))] * 4,
        compiler_params=pltpu.CompilerParams(
            collective_id=0, has_side_effects=True, vmem_limit_bytes=58 * 1024 * 1024
        ),
        name="dispatch",
    )(payload, onehot, gate_local, up_local)
    parts = shares[:, :, : 3 * choose].astype(jnp.float32)
    lane_weight = (
        parts[:, :, :choose] + parts[:, :, choose : 2 * choose] + parts[:, :, 2 * choose :]
    )
    slot_t = slot.transpose(0, 2, 1)
    share = jnp.sum(
        jnp.where(
            slot_t[:, :, :, None] == places[None, None, None, :], lane_weight[:, :, :, None], 0.0
        ),
        axis=2,
    )
    rounded = lax.reduce_precision(share, 8, 7)
    share_hi = rounded.astype(jnp.bfloat16)
    share_lo = (share - rounded).astype(jnp.bfloat16)
    return pl.pallas_call(
        functools.partial(return_kernel, n_sp, nz, min(512, width)),
        out_shape=jax.ShapeDtypeStruct((tok, width), bf),
        in_specs=[vmem] * 5,
        out_specs=vmem,
        scratch_shapes=[
            pltpu.VMEM((nz, slots, width), bf),
            pltpu.VMEM((nz, slots, width), bf),
            pltpu.VMEM((nz, n_sp, capp, width), bf),
            pltpu.VMEM((nz, n_sp, capp, width), bf),
            pltpu.VMEM((nz, tok, width), bf),
            pltpu.VMEM((nz, tok, width), bf),
            pltpu.VMEM((nz, tok, width), bf),
        ]
        + line
        + [dma((nz, n_sp))] * 2
        + [dma((nz,))] * 2,
        compiler_params=pltpu.CompilerParams(
            collective_id=1, has_side_effects=True, vmem_limit_bytes=62 * 1024 * 1024
        ),
        name="give_back",
    )(hid, down_local, share_hi, share_lo, stream)


def attention_kernel(
    n_sp, n_tp, tok, q, k, v, sink, out, k_all, v_all, k_tail, v_tail, att, got,
    t_s, t_r, a_s, a_r,
):
    sp, tp = lax.axis_index("sp"), lax.axis_index("tp")
    span, kv_cols = k.shape
    cols = q.shape[1]
    kv_local = kv_cols // HEAD
    group = cols // kv_cols
    blocks = span // WINDOW
    pieces = WINDOW // tok
    barrier = pltpu.get_barrier_semaphore()
    for d in range(1, n_tp):
        pl.semaphore_signal(
            barrier, inc=1, device_id=(sp, lax.rem(tp + d, n_tp)), device_id_type=MESH
        )

    @pl.when(sp > 0)
    def _():
        pl.semaphore_signal(barrier, inc=1, device_id=(sp - 1, tp), device_id_type=MESH)

    @pl.when(sp < n_sp - 1)
    def _():
        pl.semaphore_signal(barrier, inc=1, device_id=(sp + 1, tp), device_id_type=MESH)

    beside = jnp.where(sp > 0, 1, 0) + jnp.where(sp < n_sp - 1, 1, 0)
    pl.semaphore_wait(barrier, n_tp - 1 + beside)
    ahead = (lax.rem(sp + 1, n_sp), tp)
    last = pl.ds(span - WINDOW, WINDOW)
    tails = (
        send(k.at[last], k_tail, t_s.at[0], t_r.at[0], ahead),
        send(v.at[last], v_tail, t_s.at[1], t_r.at[1], ahead),
    )

    @pl.when(sp < n_sp - 1)
    def _():
        for copy in tails:
            copy.start()

    k_all[pl.ds(WINDOW, span), :] = k[...]
    v_all[pl.ds(WINDOW, span), :] = v[...]
    row = lax.broadcasted_iota(jnp.int32, (WINDOW, 2 * WINDOW), 0)
    col = lax.broadcasted_iota(jnp.int32, (WINDOW, 2 * WINDOW), 1)
    distance = row + WINDOW - col
    banded = (distance >= 0) & (distance < WINDOW)

    def to_owner(dest):
        at = pl.multiple_of(dest * tok, tok)
        return send(
            att.at[pl.ds(at, tok)], got.at[tp], a_s.at[dest], a_r.at[tp], (sp, dest)
        )

    def attend(i, carry):
        block = lax.rem(tp // pieces + 1 + i, blocks)

        @pl.when(block == 0)
        def _():
            @pl.when(sp > 0)
            def _():
                for copy in tails:
                    copy.wait_recv()
                k_all[pl.ds(0, WINDOW), :] = k_tail[...]
                v_all[pl.ds(0, WINDOW), :] = v_tail[...]

            @pl.when(sp == 0)
            def _():
                k_all[pl.ds(0, WINDOW), :] = jnp.zeros((WINDOW, kv_cols), jnp.bfloat16)
                v_all[pl.ds(0, WINDOW), :] = jnp.zeros((WINDOW, kv_cols), jnp.bfloat16)

        at = pl.multiple_of(block * WINDOW, WINDOW)
        start = jnp.where((sp == 0) & (block == 0), WINDOW, 0)
        allowed = banded & (col >= start)
        band = pl.ds(at, 2 * WINDOW)
        for g in range(kv_local):
            keys = k_all[band, g * HEAD : (g + 1) * HEAD]
            values = v_all[band, g * HEAD : (g + 1) * HEAD]
            heads = []
            for m in range(group):
                h = g * group + m
                query = q[pl.ds(at, WINDOW), h * HEAD : (h + 1) * HEAD]
                scores = lax.dot_general(
                    query, keys, (((1,), (1,)), ((), ())), preferred_element_type=jnp.float32
                ) * HEAD ** (-0.5)
                logits = jnp.where(allowed, scores, -jnp.inf)
                top = jnp.maximum(jnp.max(logits, axis=-1, keepdims=True), sink[h])
                raised = jnp.exp(logits - top)
                total = jnp.sum(raised, axis=-1, keepdims=True) + jnp.exp(sink[h] - top)
                probs = (raised / total).astype(jnp.bfloat16)
                heads.append(jnp.dot(probs, values, preferred_element_type=jnp.float32))
            att[pl.ds(at, WINDOW), g * group * HEAD : (g + 1) * group * HEAD] = jnp.concatenate(
                heads, axis=1
            ).astype(jnp.bfloat16)
        for piece in range(pieces):
            dest = block * pieces + piece

            @pl.when(dest != tp)
            def _():
                to_owner(dest).start()

        return carry

    lax.fori_loop(0, blocks, attend, 0)
    got[tp] = att[pl.ds(pl.multiple_of(tp * tok, tok), tok), :]
    for p in range(n_tp):
        @pl.when(tp != p)
        def _():
            send(att.at[pl.ds(0, tok)], got.at[p], a_s.at[p], a_r.at[p], (sp, p)).wait_recv()

        out[:, p * cols : (p + 1) * cols] = got[p]
    for p in range(n_tp):
        @pl.when(tp != p)
        def _():
            to_owner(p).wait_send()

    @pl.when(sp < n_sp - 1)
    def _():
        for copy in tails:
            copy.wait_send()


def attend_tokens(query_heads, key_heads, value_heads, sink_logit, tok):
    n_sp, n_tp = lax.axis_size("sp"), lax.axis_size("tp")
    span, cols = query_heads.shape
    kv_cols = key_heads.shape[1]
    vmem = pl.BlockSpec(memory_space=pltpu.VMEM)
    dma = pltpu.SemaphoreType.DMA
    bf = jnp.bfloat16
    return pl.pallas_call(
        functools.partial(attention_kernel, n_sp, n_tp, tok),
        out_shape=jax.ShapeDtypeStruct((tok, n_tp * cols), bf),
        in_specs=[vmem] * 3 + [pl.BlockSpec(memory_space=pltpu.SMEM)],
        out_specs=vmem,
        scratch_shapes=[
            pltpu.VMEM((span + WINDOW, kv_cols), bf),
            pltpu.VMEM((span + WINDOW, kv_cols), bf),
            pltpu.VMEM((WINDOW, kv_cols), bf),
            pltpu.VMEM((WINDOW, kv_cols), bf),
            pltpu.VMEM((span, cols), bf),
            pltpu.VMEM((n_tp, tok, cols), bf),
            dma((2,)),
            dma((2,)),
            dma((n_tp,)),
            dma((n_tp,)),
        ],
        compiler_params=pltpu.CompilerParams(
            collective_id=2, has_side_effects=True, vmem_limit_bytes=24 * 1024 * 1024
        ),
        name="attend",
    )(query_heads, key_heads, value_heads, sink_logit)


def local(
    query_heads,
    key_heads,
    value_heads,
    sink_logit,
    residual,
    out_weight,
    norm_gain,
    routes,
    route_weight,
    gate_weight,
    up_weight,
    down_weight,
):
    sp_count = lax.axis_size("sp")
    tok_rows = residual.shape[0]
    token_heads = attend_tokens(query_heads, key_heads, value_heads, sink_logit, tok_rows)
    mixed = jnp.dot(token_heads, out_weight, preferred_element_type=jnp.float32)
    stream = (residual.astype(jnp.float32) + mixed).astype(jnp.bfloat16)
    stream32 = stream.astype(jnp.float32)
    normed = (
        stream32
        * lax.rsqrt(jnp.mean(stream32 * stream32, axis=-1, keepdims=True) + eps)
        * norm_gain
    ).astype(jnp.bfloat16)
    choose_count = routes.shape[1]
    capacity = max(2, 5 * tok_rows * choose_count // (4 * sp_count))
    return experts(
        normed, stream, routes, route_weight, gate_weight[0], up_weight[0], down_weight[0], capacity
    )


def solution(mesh):
    placed = (
        P("sp", "tp"),
        P("sp", "tp"),
        P("sp", "tp"),
        P("tp"),
        P(("sp", "tp"), None),
        P(),
        P(),
        P("sp", None),
        P(("sp", "tp"), None),
        P("sp", None, "tp"),
        P("sp", None, "tp"),
        P("sp", "tp", None),
    )
    return jax.shard_map(
        local, mesh=mesh, in_specs=placed, out_specs=P(("sp", "tp"), None), check_vma=False
    )
```
